32 devices in a mesh: ep: 4 (over y, x), tp: 8 (over z, core).
Axes of the slice: x: 2, y: 2, z: 4, core: 2. Of those that a mesh axis runs over, the one named last changes fastest.
Arguments:
- queries: bfloat16 [16, 64, 2, 512], P('tp', None, None, 'ep'), may hold values from -24 to 24
- key_vectors: bfloat16 [16, 64, 2, 512], P('tp', None, None, 'ep'), may hold values from -24 to 24
- value_vectors: bfloat16 [16, 64, 2, 512], P('tp', None, None, 'ep'), may hold values from -6 to 6
- mixer_weight: bfloat16 [1024, 2048], replicated, may hold values from -0.375 to 0.375
- expert_rows: bfloat16 [512, 2048], P('ep'), may hold values from -6 to 6
- norm_gain: float32 [2048], replicated, may hold values from 0.1 to 1.9
- route_ids: int32 [512, 2], P('ep'), may hold values from 0 to 7, all different within a row; in each aligned block of 128 rows (0 to 127, 128 to 255, ...) at most 64 rows name the same one
- route_logits: float32 [512, 2], P('ep'), may hold values from -4 to 4
- gate_weight: bfloat16 [8, 2048, 4096], P('ep', None, 'tp'), may hold values from -0.39648438 to 0.39648438
- up_weight: bfloat16 [8, 2048, 4096], P('ep', None, 'tp'), may hold values from -0.39648438 to 0.39648438
- down_weight: bfloat16 [8, 4096, 2048], P('ep', 'tp'), may hold values from -0.028076172 to 0.028076172
Outputs:
- mixer_out: bfloat16 [2, 512, 2048], P(None, ('ep', 'tp'))
- routed_out: bfloat16 [2048, 512], P('tp', 'ep')
The draws below stay inside these ranges and needn't reach their ends.
Inputs may be any that keep to these rules, and one draw needn't show every extreme that they name: `route_ids`: each row names 2 different experts. Among the 128 rows of one index of ep no expert is named more than 64 times, a bound that some expert reaches in such a block.
All inputs are finite; a program needn't handle non-finite values.
Results may differ from the reference program's by a relative error of at most 0.018.
Values may be sent and summed in bfloat16 or wider, within the bound.
A program may use at most 64 MiB of HBM per device.

```python
import math
import jax
import jax.numpy as jnp
import numpy as np
from jax import lax

D = 2048
HEADS = 16
HD = 64
FF = 4096
TOP = 2
SEQS = 2
SEG = 128
B_EP = 128
EXPERTS = 8
FF_DEV = 512
CAP = 64
LEN = 512
TOKENS_B = 512
N_EP = 4
N_TP = 8


def head_axes(key):
    direction = jax.random.normal(jax.random.fold_in(key, 101), (HEADS, HD), jnp.float32)
    return direction / jnp.sqrt(jnp.sum(direction * direction, axis=1, keepdims=True))


def noise_draw(key, array_shape):
    return jnp.clip(jax.random.normal(key, array_shape, jnp.float32), -4.0, 4.0)


def draw_queries(key, part):
    direction = head_axes(key)
    noise_part = noise_draw(jax.random.fold_in(key, 1), (HEADS, HD, SEQS, LEN))
    return (math.sqrt(HD) * direction[:, :, None, None] + noise_part).astype(jnp.bfloat16)


def draw_key_vectors(key, part):
    direction = head_axes(key)
    slow_rate = math.log(LEN) + 3.0
    fast_heads = jax.random.randint(jax.random.fold_in(key, 103), (HEADS,), 0, 2)
    reference_level = jnp.where(fast_heads > 0, 5.0, slow_rate).astype(jnp.float32)
    noise_perturbation = jax.random.uniform(jax.random.fold_in(key, 105), (HEADS, SEQS, LEN // SEG), jnp.float32, -0.7, 0.7)
    noise_perturbation = jnp.repeat(noise_perturbation, SEG, axis=2)
    element_locations = jax.random.randint(jax.random.fold_in(key, 107), (HEADS, SEQS, 3), 0, LEN)
    target_slot_numbers = jnp.arange(LEN, dtype=jnp.int32)
    spike_location = jnp.any(target_slot_numbers[None, None, :, None] == element_locations[:, :, None, :], axis=3)
    lookup_occurrence = jnp.where(spike_location, 0.5, reference_level[:, None, None] + noise_perturbation)
    noise_part = noise_draw(jax.random.fold_in(key, 2), (HEADS, HD, SEQS, LEN))
    return (noise_part - lookup_occurrence[:, None, :, :] * direction[:, :, None, None]).astype(jnp.bfloat16)


def raised(result, key, source, target, shards_of, factor):
    def block_of(dim):
        return (jnp.arange(result.shape[dim]) // (result.shape[dim] // shards_of)).reshape((-1,) + (1,) * (result.ndim - 1 - dim))

    one_side = jax.random.permutation(key, shards_of)[block_of(target)]
    second = (block_of(target) + shards_of // 2) % shards_of
    return jnp.where((block_of(source) == one_side) | (block_of(source) == second), factor * result, result)


def block_levels(stream_key, extent, cuts, smallest, top_value):
    level = 1.0
    for dim, blocks in cuts:
        draws = jax.random.uniform(jax.random.fold_in(jax.random.fold_in(stream_key, 6), dim), (blocks,), jnp.float32, smallest / len(cuts), top_value / len(cuts))
        level = level * jnp.repeat(jnp.exp(draws), extent[dim] // blocks).reshape((-1,) + (1,) * (len(extent) - 1 - dim))
    return level


def deal_out(own_key, own, number, rows, count, top, most, slope):
    order = jax.random.permutation(own_key, count)
    crowded, usual = portions_of(count, rows * top, most, slope, True), portions_of(count, rows * top, most, slope, False)
    places = jnp.arange(count)

    def named(sizes, rotation):
        used = int((sizes > 0).sum())
        fixed = max(1, used // 4)
        passed = fixed + (places - fixed + rotation * (used - fixed)) % max(1, count - fixed)
        return jnp.zeros((count,), jnp.int32).at[order[jnp.where(places < fixed, places, passed)]].set(jnp.asarray(sizes, jnp.int32))

    sizes = jnp.where(number % 4 == 0, named(crowded, number // 4), named(usual, number - number // 4 - 1))
    mixed = jax.random.permutation(jax.random.fold_in(own, 3), count)
    donor, taker = mixed[0:count // 2 * 2:2], mixed[1:count // 2 * 2:2]
    margin = jnp.minimum(sizes[donor] - 1, most - sizes[taker]) // 2
    margin = jnp.where((donor == order[0]) | (taker == order[0]) | (sizes[taker] == 0), 0, jnp.maximum(margin, 0))
    passed = jax.random.randint(jax.random.fold_in(own, 4), (count // 2,), 0, 1 << 20) % (margin + 1)
    sizes = sizes.at[donor].add(-passed).at[taker].add(passed)
    items = jnp.searchsorted(jnp.cumsum(sizes), jnp.arange(rows * top), side="right").astype(jnp.int32)
    table = items.reshape(top, rows).T
    table = table[jax.random.permutation(jax.random.fold_in(own, 1), rows)]
    rotation = jax.random.randint(jax.random.fold_in(own, 2), (rows, 1), 0, top)
    return jnp.take_along_axis(table, (jnp.arange(top)[None, :] + rotation) % top, axis=1)


def portions_of(number_of, total, most, slope, full):
    loads = [(1 << 20) // math.isqrt(grade ** slope) + 1 for grade in range(1, number_of + 1)]
    largest = most if full else min(most, max(-(-total // number_of), total * loads[0] // sum(loads)))
    least = 1 if total - largest >= number_of - 1 else 0
    given, rest = [largest] + [least] * (number_of - 1), total - largest - least * (number_of - 1)
    while rest > 0:
        movable = [i for i in range(1, number_of) if given[i] < largest] or [i for i in range(1, number_of) if given[i] < most]
        mass, left = sum([loads[i] for i in movable]), rest
        for i in movable:
            extra = min(most - given[i], max(1, left * loads[i] // mass), rest)
            given[i] = given[i] + extra
            rest = rest - extra
    return np.array(given)


def normal_values(key, extent, width, bound, split=(), held_as=jnp.bfloat16):
    result = jax.random.normal(key, extent, jnp.float32) * width
    if len(split) > 0:
        result = block_levels(key, extent, split, -0.22, 0.18) * result
    return jnp.clip(result, min=-bound, max=bound).astype(held_as)


def noise_with(stream_key, extent, width, most, cuts, heavy, kind=jnp.bfloat16):
    values = width * jax.random.normal(stream_key, extent, jnp.float32)
    if cuts:
        values = values * block_levels(stream_key, extent, cuts, -0.22, 0.18)
    return jnp.clip(raised(values, jax.random.fold_in(stream_key, 3), *heavy), -most, most).astype(kind)


def setup_inputs(seed: int = 0) -> dict:
    key_of = jax.random.split(jax.random.key(seed), 12)
    queries = draw_queries(jax.random.fold_in(key_of[11], 71), 0)
    key_vectors = draw_key_vectors(jax.random.fold_in(key_of[11], 71), 0)
    value_vectors = normal_values(key_of[2], (HEADS, HD, SEQS, LEN), 1.0, 6.0, ((0, 8), (3, 4)))
    mixer_weight = normal_values(key_of[3], (HEADS * HD, D), (HEADS * HD // 4) ** -0.5, 0.375)
    expert_rows = normal_values(key_of[4], (TOKENS_B, D), 1.0, 6.0, ((0, 4),))
    norm_gain = jnp.clip(1.0 + 0.18 * jax.random.normal(key_of[5], (D,), jnp.float32), 0.1, 1.9)
    route_ids_keys = jax.random.split(jax.random.fold_in(key_of[6], 1), TOKENS_B // B_EP)
    route_ids_turns = jax.random.permutation(jax.random.fold_in(key_of[6], 3), TOKENS_B // B_EP)
    route_ids = jax.vmap(lambda own, number: deal_out(jax.random.fold_in(key_of[6], 2), own, number, B_EP, EXPERTS, TOP, CAP, 2))(route_ids_keys, route_ids_turns).reshape((TOKENS_B, TOP))
    route_logits = normal_values(key_of[7], (TOKENS_B, TOP), 1.0, 4.0, ((0, 4),), jnp.float32)
    gate_weight = normal_values(key_of[8], (EXPERTS, D, FF), (3.0 * D ** -0.5), 0.39648438, ((0, 4), (2, 8)))
    up_weight = normal_values(key_of[9], (EXPERTS, D, FF), (3.0 * D ** -0.5), 0.39648438, ((0, 4), (2, 8)))
    down_weight = noise_with(key_of[10], (EXPERTS, FF, D), (0.3 * FF ** -0.5), 0.028076172, ((0, 4), (1, 8)), (1, 2, 8, 2.0))
    return {"queries": queries, "key_vectors": key_vectors, "value_vectors": value_vectors, "mixer_weight": mixer_weight, "expert_rows": expert_rows, "norm_gain": norm_gain, "route_ids": route_ids, "route_logits": route_logits, "gate_weight": gate_weight, "up_weight": up_weight, "down_weight": down_weight}


limit_value = 7.0
alpha_value = 1.702
norm_eps = 1e-06

def activate(gate_pre, up_pre):
    gate_clamped = jnp.minimum(gate_pre, limit_value)
    up_clamped = jnp.clip(up_pre, -limit_value, limit_value)
    return ((up_clamped + 1.0) * gate_clamped * jax.nn.sigmoid(alpha_value * gate_clamped)).astype(jnp.bfloat16)

def stick_block(query_part, key_part, value_part, query_start):
    scores = jnp.einsum('hdq,hdk->hqk', query_part.astype(jnp.float32), key_part.astype(jnp.float32)) * HD ** (-0.5)
    query_pos = query_start + lax.broadcasted_iota(jnp.int32, (SEG, LEN), 0)
    lookup_slot = lax.broadcasted_iota(jnp.int32, (SEG, LEN), 1)
    usable = (lookup_slot < query_pos)[None]
    log_keep = jnp.where(usable, jax.nn.log_sigmoid(-scores), 0.0)
    blocked = log_keep.reshape(HEADS, SEG, N_EP, SEG)
    within = lax.cumsum(blocked, axis=3, reverse=True) - blocked
    block_totals = lax.optimization_barrier(jnp.sum(blocked, axis=3))
    log_beta = jax.nn.log_sigmoid(scores).reshape(HEADS, SEG, N_EP, SEG)
    weight = jnp.where(usable.reshape(1, SEG, N_EP, SEG), jnp.exp(log_beta + within), 0.0).astype(jnp.bfloat16)
    block_values = jnp.einsum('hqbk,hdbk->hdqb', weight.astype(jnp.float32), value_part.reshape(HEADS, HD, N_EP, SEG).astype(jnp.float32))
    later_sums = lax.cumsum(block_totals, axis=2, reverse=True) - block_totals
    return lax.optimization_barrier(jnp.sum(jnp.exp(later_sums)[:, None] * block_values, axis=3)).astype(jnp.bfloat16)

def reference(queries, key_vectors, value_vectors, mixer_weight, expert_rows, norm_gain, route_ids, route_logits, gate_weight, up_weight, down_weight):

    def one_block(block_number):
        seq_index = block_number // N_EP
        query_start = (block_number % N_EP * SEG).astype(jnp.int32)
        query_seq = lax.dynamic_index_in_dim(queries, seq_index, 2, keepdims=False)
        query_part = lax.dynamic_slice_in_dim(query_seq, query_start, SEG, 2)
        key_part = lax.dynamic_index_in_dim(key_vectors, seq_index, 2, keepdims=False)
        value_part = lax.dynamic_index_in_dim(value_vectors, seq_index, 2, keepdims=False)
        return stick_block(query_part, key_part, value_part, query_start)
    attended = lax.map(one_block, jnp.arange(SEQS * N_EP, dtype=jnp.int32))
    attended = attended.reshape(SEQS, N_EP, HEADS, HD, SEG).transpose(0, 1, 4, 2, 3).reshape(SEQS, LEN, HEADS * HD)
    mixer_out = jnp.einsum('slc,cm->slm', attended.astype(jnp.float32), mixer_weight.astype(jnp.float32)).astype(jnp.bfloat16)
    values = expert_rows.astype(jnp.float32)
    scaled = values * lax.rsqrt(lax.optimization_barrier(jnp.mean(values * values, axis=-1, keepdims=True)) + norm_eps)
    normed = (scaled * norm_gain).astype(jnp.bfloat16)
    route_weight = jax.nn.softmax(route_logits, axis=-1)
    block_ids = route_ids.reshape(N_EP, B_EP * TOP)
    one_hot_matrix = (block_ids[:, :, None] == jnp.arange(EXPERTS, dtype=jnp.int32)[None, None, :]).astype(jnp.int32)
    earlier = jnp.cumsum(one_hot_matrix, axis=1) - one_hot_matrix
    slot_rank = lax.optimization_barrier(jnp.sum(earlier * one_hot_matrix, axis=2))
    source = jnp.arange(N_EP, dtype=jnp.int32)[:, None]
    token_index = source * B_EP + jnp.arange(B_EP * TOP, dtype=jnp.int32)[None, :] // TOP
    table_index = ((block_ids * N_EP + source) * CAP + slot_rank).reshape(-1).astype(jnp.int32)
    owner_token = jnp.zeros((EXPERTS * N_EP * CAP,), jnp.int32).at[table_index].set(token_index.reshape(-1))
    slot_rows = N_EP * CAP

    def one_expert(expert_index):
        owners = lax.dynamic_slice_in_dim(owner_token, expert_index * slot_rows, slot_rows)
        rows_in = normed[owners]
        gate_pre = jnp.dot(rows_in, lax.dynamic_index_in_dim(gate_weight, expert_index, 0, keepdims=False), preferred_element_type=jnp.float32)
        up_pre = jnp.dot(rows_in, lax.dynamic_index_in_dim(up_weight, expert_index, 0, keepdims=False), preferred_element_type=jnp.float32)
        hidden = activate(gate_pre, up_pre)
        down_part = lax.dynamic_index_in_dim(down_weight, expert_index, 0, keepdims=False)
        group_part = jnp.einsum('rgf,gfd->grd', hidden.reshape(slot_rows, N_TP, FF_DEV).astype(jnp.float32), down_part.reshape(N_TP, FF_DEV, D).astype(jnp.float32))
        rounded = lax.optimization_barrier(group_part.astype(jnp.bfloat16))
        return lax.optimization_barrier(jnp.sum(rounded.astype(jnp.float32), axis=0))
    expert_value = lax.map(one_expert, jnp.arange(EXPERTS, dtype=jnp.int32)).reshape(EXPERTS * slot_rows, D)
    picked = expert_value[table_index].reshape(TOKENS_B, TOP, D)
    combined = lax.optimization_barrier(jnp.sum(picked * route_weight[:, :, None], axis=1))
    routed_out = combined.T.astype(jnp.bfloat16)
    return (mixer_out, routed_out)
```

```python
import functools

import jax
import jax.numpy as jnp
from jax import lax
from jax.experimental import pallas as pl
from jax.experimental.pallas import tpu as pltpu
from jax.sharding import PartitionSpec as P

limit_value = 7.0
alpha_value = 1.702
norm_eps = 1e-06

MESH = pl.DeviceIdType.MESH
f32 = jnp.float32
bf16 = jnp.bfloat16


def activate(gate_pre, up_pre):
    g = jnp.minimum(gate_pre, limit_value)
    u = jnp.clip(up_pre, -limit_value, limit_value)
    return ((u + 1.0) * g / (1.0 + jnp.exp(-alpha_value * g))).astype(bf16)


def partner_of(me, offset, count):
    other = me
    bit = 1
    while bit < count:
        set_bit = (offset // bit) % 2
        other = other + set_bit * bit * (1 - 2 * ((me // bit) % 2))
        bit *= 2
    return other


def kernel(
    n_ep,
    n_tp,
    qt_ref,
    kv_ref,
    x_ref,
    gain_ref,
    wt_ref,
    gate_hbm,
    up_hbm,
    down_hbm,
    mixer_hbm,
    mix_out,
    routed_out,
    wg,
    wu,
    wd,
    wm,
    xr,
    wr,
    xn,
    kvr,
    pb,
    cr,
    sb,
    rr,
    zb,
    zr,
    at_send,
    at_recv,
    w_sem,
    x_ss,
    x_rs,
    wt_ss,
    wt_rs,
    f_ss,
    f_rs,
    kv_ss,
    kv_rs,
    c_ss,
    c_rs,
    r_ss,
    r_rs,
    z_ss,
    z_rs,
    a_ss,
    a_rs,
):
    e = lax.axis_index("ep")
    t = lax.axis_index("tp")
    core = t % 2
    zi = t // 2
    zs = n_tp // 2
    mate = t + 1 - 2 * core
    heads, seqs, seg, hd = qt_ref.shape
    tokens, width = x_ref.shape
    half = tokens // 2
    local_experts = wg.shape[0]
    ch = width // n_tp
    pp = seg // n_tp

    weights = [
        pltpu.make_async_copy(src, dst, w_sem.at[i])
        for i, (src, dst) in enumerate(
            ((gate_hbm, wg), (up_hbm, wu), (down_hbm, wd), (mixer_hbm, wm))
        )
    ]
    for copy in weights:
        copy.start()

    def ep_peer(d):
        return partner_of(e, d, n_ep)

    barrier = pltpu.get_barrier_semaphore()
    for d in range(1, n_ep):
        pl.semaphore_signal(barrier, inc=1, device_id={"ep": ep_peer(d)}, device_id_type=MESH)
    for d in range(1, n_tp):
        pl.semaphore_signal(
            barrier, inc=1, device_id={"tp": (t + d) % n_tp}, device_id_type=MESH
        )
    pl.semaphore_wait(barrier, n_ep - 1 + n_tp - 1)

    mine = pl.ds(pl.multiple_of(core * half, half), half)

    def x_copy(d):
        return pltpu.make_async_remote_copy(
            src_ref=x_ref.at[mine],
            dst_ref=xr.at[d, mine],
            send_sem=x_ss.at[d],
            recv_sem=x_rs.at[d],
            device_id={"ep": ep_peer(d)},
            device_id_type=MESH,
        )

    def wt_copy(d):
        return pltpu.make_async_remote_copy(
            src_ref=wt_ref.at[ep_peer(d)],
            dst_ref=wr.at[d],
            send_sem=wt_ss.at[d],
            recv_sem=wt_rs.at[d],
            device_id={"ep": ep_peer(d)},
            device_id_type=MESH,
        )

    def f_copy(d):
        return pltpu.make_async_remote_copy(
            src_ref=xr.at[d, mine],
            dst_ref=xr.at[d, mine],
            send_sem=f_ss.at[d],
            recv_sem=f_rs.at[d],
            device_id={"tp": mate},
            device_id_type=MESH,
        )

    def kv_copy(d):
        return pltpu.make_async_remote_copy(
            src_ref=kv_ref,
            dst_ref=kvr.at[d],
            send_sem=kv_ss.at[d],
            recv_sem=kv_rs.at[d],
            device_id={"ep": (e + d) % n_ep},
            device_id_type=MESH,
        )

    def c_copy(d):
        return pltpu.make_async_remote_copy(
            src_ref=pb.at[d, 1 - core],
            dst_ref=cr.at[d],
            send_sem=c_ss.at[d],
            recv_sem=c_rs.at[d],
            device_id={"tp": mate},
            device_id_type=MESH,
        )

    def r_copy(d):
        return pltpu.make_async_remote_copy(
            src_ref=sb.at[d],
            dst_ref=rr.at[d],
            send_sem=r_ss.at[d],
            recv_sem=r_rs.at[d],
            device_id={"ep": ep_peer(d)},
            device_id_type=MESH,
        )

    def z_copy(d):
        dz = (zi + d) % zs
        return pltpu.make_async_remote_copy(
            src_ref=zb.at[dz],
            dst_ref=zr.at[d],
            send_sem=z_ss.at[d],
            recv_sem=z_rs.at[d],
            device_id={"tp": dz * 2 + core},
            device_id_type=MESH,
        )

    def a_copy(d):
        to = (t + d) % n_tp
        return pltpu.make_async_remote_copy(
            src_ref=at_send.at[to],
            dst_ref=at_recv.at[t],
            send_sem=a_ss.at[d],
            recv_sem=a_rs.at[d],
            device_id={"tp": to},
            device_id_type=MESH,
        )

    for d in range(1, n_ep):
        wt_copy(d).start()
        x_copy(d).start()
    for d in range(1, n_ep):

        @pl.when(e + d < n_ep)
        def _():
            kv_copy(d).start()

    def normalize(rows_ref):
        values = rows_ref[...].astype(f32)
        mean = jnp.mean(values * values, axis=-1, keepdims=True)
        xn[...] = (values * lax.rsqrt(mean + norm_eps) * gain_ref[...]).astype(bf16)

    def experts(d, route):
        columns = route.T
        hidden = []
        for j in range(local_experts):
            gate_pre = jnp.dot(xn[...], wg[j], preferred_element_type=f32)
            up_pre = jnp.dot(xn[...], wu[j], preferred_element_type=f32)
            hidden.append(activate(gate_pre, up_pre))
        for c in range(n_tp):
            total = None
            for j in range(local_experts):
                term = columns[:, j : j + 1] * jnp.dot(
                    hidden[j], wd[j, :, c * ch : (c + 1) * ch], preferred_element_type=f32
                )
                total = term if total is None else total + term
            pb[d, c % 2, c // 2] = total.astype(bf16)

    def finish(d):
        c_copy(d).wait_recv()
        sb[d] = (pb[d, core].astype(f32) + cr[d].astype(f32)).astype(bf16)

    normalize(x_ref)
    for copy in weights[:3]:
        copy.wait()
    experts(0, wt_ref[e])
    c_copy(0).start()

    def step(d, carry):
        x_copy(d).wait_recv()
        f_copy(d).start()
        finish(d - 1)

        @pl.when(d > 1)
        def _():
            r_copy(d - 1).start()

        f_copy(d).wait_recv()
        wt_copy(d).wait_recv()
        normalize(xr.at[d])
        experts(d, wr[d])
        c_copy(d).start()
        return carry

    lax.fori_loop(1, n_ep, step, 0)
    finish(n_ep - 1)
    r_copy(n_ep - 1).start()

    pairs = heads * seqs
    row_id = lax.broadcasted_iota(jnp.int32, (seg, seg), 0)
    col_id = lax.broadcasted_iota(jnp.int32, (seg, seg), 1)
    later_mask = (row_id > col_id).astype(f32).astype(bf16)
    scale = hd ** (-0.5)

    def block(kv, diagonal):
        outs = []
        for p in range(pairs):
            h, s = p // seqs, p % seqs
            scores = jnp.dot(qt_ref[h, s], kv[0, h, s], preferred_element_type=f32) * scale
            log_term = jnp.log(1.0 + jnp.exp(-jnp.abs(scores)))
            keep = -(jnp.maximum(scores, 0.0) + log_term)
            beta = jnp.minimum(scores, 0.0) - log_term
            if diagonal:
                keep = jnp.where(col_id < row_id, keep, 0.0)
            high = keep.astype(bf16)
            low = (keep - high.astype(f32)).astype(bf16)
            within = jnp.dot(high, later_mask, preferred_element_type=f32) + jnp.dot(
                low, later_mask, preferred_element_type=f32
            )
            weight = jnp.exp(beta + within)
            if diagonal:
                weight = jnp.where(col_id < row_id, weight, 0.0)
            out = lax.dot_general(
                weight.astype(bf16),
                kv[1, h, s],
                (((1,), (1,)), ((), ())),
                preferred_element_type=f32,
            )
            outs.append((out, jnp.sum(keep, axis=1, keepdims=True)))
        return outs

    first = block(kv_ref, True)
    state = []
    for out, total in first:
        state.extend((out, total))

    def further(d, state):
        pltpu.make_async_remote_copy(
            src_ref=kv_ref,
            dst_ref=kvr.at[d],
            send_sem=kv_ss.at[d],
            recv_sem=kv_rs.at[d],
            device_id={"ep": (e + d) % n_ep},
            device_id_type=MESH,
        ).wait_recv()
        fresh = []
        for p, (out, total) in enumerate(block(kvr.at[d], False)):
            so_far, later = state[2 * p], state[2 * p + 1]
            fresh.extend((so_far + jnp.exp(later) * out, later + total))
        return tuple(fresh)

    state = lax.fori_loop(1, e + 1, further, tuple(state))
    for p in range(pairs):
        h, s = p // seqs, p % seqs
        attended = state[2 * p]
        for c in range(n_tp):
            at_send[c, s * pp : (s + 1) * pp, h * hd : (h + 1) * hd] = attended[
                c * pp : (c + 1) * pp
            ].astype(bf16)
    for d in range(1, n_tp):
        a_copy(d).start()

    for d in range(1, n_ep):
        r_copy(d).wait_recv()
    for c in range(zs):
        total = sb[0, c].astype(f32)
        for d in range(1, n_ep):
            total = total + rr[d, c].astype(f32)
        zb[c] = total.astype(bf16)
    for d in range(1, zs):
        z_copy(d).start()

    weights[3].wait()
    at_recv[t] = at_send[t]
    for d in range(1, n_tp):
        pltpu.make_async_remote_copy(
            src_ref=at_send.at[t],
            dst_ref=at_recv.at[(t + n_tp - d) % n_tp],
            send_sem=a_ss.at[d],
            recv_sem=a_rs.at[d],
            device_id={"tp": (t + d) % n_tp},
            device_id_type=MESH,
        ).wait_recv()
    channels = heads * hd
    wide = jnp.concatenate([at_recv[c] for c in range(n_tp)], axis=1)
    mixed = jnp.dot(wide, wm[...], preferred_element_type=f32)
    for s in range(seqs):
        mix_out[s] = mixed[s * pp : (s + 1) * pp].astype(bf16)

    total = zb[zi].astype(f32)
    for d in range(1, zs):
        z_copy(d).wait_recv()
        total = total + zr[d].astype(f32)
    routed_out[...] = total.T.astype(bf16)

    for d in range(1, n_ep):
        x_copy(d).wait_send()
        wt_copy(d).wait_send()
        f_copy(d).wait_send()
        r_copy(d).wait_send()

        @pl.when(e + d < n_ep)
        def _():
            kv_copy(d).wait_send()

    for d in range(n_ep):
        c_copy(d).wait_send()
    for d in range(1, zs):
        z_copy(d).wait_send()
    for d in range(1, n_tp):
        a_copy(d).wait_send()


def body(
    queries,
    key_vectors,
    value_vectors,
    mixer_weight,
    expert_rows,
    norm_gain,
    route_ids,
    route_logits,
    gate_weight,
    up_weight,
    down_weight,
):
    n_ep, n_tp = lax.axis_size("ep"), lax.axis_size("tp")
    heads, hd, seqs, seg = queries.shape
    tokens, width = expert_rows.shape
    local_experts, _, ff = gate_weight.shape
    zs, ch, pp = n_tp // 2, width // n_tp, seg // n_tp

    qt = queries.transpose(0, 2, 3, 1)
    kv = jnp.stack([key_vectors, value_vectors]).transpose(0, 1, 3, 2, 4)
    route_weight = jax.nn.softmax(route_logits, axis=-1)
    slots = 8 * -(-local_experts // 8)
    expert = (
        jnp.arange(n_ep, dtype=jnp.int32)[:, None] * local_experts
        + jnp.arange(slots, dtype=jnp.int32)[None, :]
    )
    inside = jnp.arange(slots, dtype=jnp.int32)[None, :, None] < local_experts
    table = 0.0
    for k in range(route_ids.shape[1]):
        hit = jnp.logical_and(route_ids[:, k][None, None, :] == expert[:, :, None], inside)
        table = table + jnp.where(hit, route_weight[:, k][None, None, :], 0.0)

    vmem = pl.BlockSpec(memory_space=pltpu.VMEM)
    anywhere = pl.BlockSpec(memory_space=pl.ANY)
    dma = pltpu.SemaphoreType.DMA
    return pl.pallas_call(
        functools.partial(kernel, n_ep, n_tp),
        out_shape=(
            jax.ShapeDtypeStruct((seqs, pp, width), bf16),
            jax.ShapeDtypeStruct((ch, tokens), bf16),
        ),
        in_specs=[vmem] * 5 + [anywhere] * 4,
        out_specs=(vmem, vmem),
        scratch_shapes=[
            pltpu.VMEM(gate_weight.shape, bf16),
            pltpu.VMEM(up_weight.shape, bf16),
            pltpu.VMEM(down_weight.shape, bf16),
            pltpu.VMEM(mixer_weight.shape, bf16),
            pltpu.VMEM((n_ep, tokens, width), bf16),
            pltpu.VMEM((n_ep, slots, tokens), f32),
            pltpu.VMEM((tokens, width), bf16),
            pltpu.VMEM((n_ep,) + kv.shape, bf16),
            pltpu.VMEM((n_ep, 2, zs, tokens, ch), bf16),
            pltpu.VMEM((n_ep, zs, tokens, ch), bf16),
            pltpu.VMEM((n_ep, zs, tokens, ch), bf16),
            pltpu.VMEM((n_ep, zs, tokens, ch), bf16),
            pltpu.VMEM((zs, tokens, ch), bf16),
            pltpu.VMEM((zs, tokens, ch), bf16),
            pltpu.VMEM((n_tp, seqs * pp, heads * hd), bf16),
            pltpu.VMEM((n_tp, seqs * pp, heads * hd), bf16),
            dma((4,)),
        ]
        + [dma((n_ep,))] * 12
        + [dma((zs,))] * 2
        + [dma((n_tp,))] * 2,
        compiler_params=pltpu.CompilerParams(
            collective_id=0, has_side_effects=True, vmem_limit_bytes=60 * 1024 * 1024
        ),
    )(
        qt,
        kv,
        expert_rows,
        norm_gain[None, :],
        table,
        gate_weight,
        up_weight,
        down_weight,
        mixer_weight,
    )


def solution(mesh):
    in_specs = (
        P("tp", None, None, "ep"),
        P("tp", None, None, "ep"),
        P("tp", None, None, "ep"),
        P(),
        P("ep", None),
        P(),
        P("ep", None),
        P("ep", None),
        P("ep", None, "tp"),
        P("ep", None, "tp"),
        P("ep", "tp", None),
    )
    out_specs = (P(None, ("ep", "tp"), None), P("tp", "ep"))
    return jax.shard_map(body, mesh=mesh, in_specs=in_specs, out_specs=out_specs, check_vma=False)
```

```python
import functools

import jax
import jax.numpy as jnp
from jax import lax
from jax.experimental import pallas as pl
from jax.experimental.pallas import tpu as pltpu
from jax.sharding import PartitionSpec as P

limit_value = 7.0
alpha_value = 1.702
norm_eps = 1e-06

MESH = pl.DeviceIdType.MESH
f32 = jnp.float32
bf16 = jnp.bfloat16


def activate(gate_pre, up_pre):
    g = jnp.minimum(gate_pre, limit_value)
    u = jnp.clip(up_pre, -limit_value, limit_value)
    return ((u + 1.0) * g / (1.0 + jnp.exp(-alpha_value * g))).astype(bf16)


def partner_of(me, offset, count):
    other = me
    bit = 1
    while bit < count:
        set_bit = (offset // bit) % 2
        other = other + set_bit * bit * (1 - 2 * ((me // bit) % 2))
        bit *= 2
    return other


def kernel(
    n_ep,
    n_tp,
    q_ref,
    k_ref,
    v_ref,
    x_ref,
    gain_ref,
    ids_ref,
    logits_ref,
    gate_hbm,
    up_hbm,
    down_hbm,
    mixer_hbm,
    mix_out,
    routed_out,
    wg,
    wu,
    wd,
    wm,
    xr,
    wr,
    xn,
    kvr,
    pb,
    cr,
    sb,
    rr,
    zb,
    zr,
    at_send,
    at_recv,
    qt_ref,
    kv_ref,
    wt_ref,
    acc,
    tot,
    w_sem,
    x_ss,
    x_rs,
    wt_ss,
    wt_rs,
    g_ss,
    g_rs,
    f_ss,
    f_rs,
    kv_ss,
    kv_rs,
    c_ss,
    c_rs,
    r_ss,
    r_rs,
    z_ss,
    z_rs,
    a_ss,
    a_rs,
):
    e = lax.axis_index("ep")
    t = lax.axis_index("tp")
    core = t % 2
    zi = t // 2
    zs = n_tp // 2
    mate = t + 1 - 2 * core
    heads, seqs, seg, hd = qt_ref.shape
    tokens, width = x_ref.shape
    half = tokens // 2
    quarter = tokens // 4
    zp = zi % 2
    zmate = t + 2 - 4 * zp
    slots = wt_ref.shape[1]
    local_experts = wg.shape[0]
    ch = width // n_tp
    pp = seg // n_tp

    weights = [
        pltpu.make_async_copy(src, dst, w_sem.at[i])
        for i, (src, dst) in enumerate(
            ((gate_hbm, wg), (up_hbm, wu), (down_hbm, wd), (mixer_hbm, wm))
        )
    ]
    for copy in weights:
        copy.start()

    def ep_peer(d):
        return partner_of(e, d, n_ep)

    barrier = pltpu.get_barrier_semaphore()
    for d in range(1, n_ep):
        pl.semaphore_signal(barrier, inc=1, device_id={"ep": ep_peer(d)}, device_id_type=MESH)
    for d in range(1, n_tp):
        pl.semaphore_signal(
            barrier, inc=1, device_id={"tp": (t + d) % n_tp}, device_id_type=MESH
        )

    rows = hd * seqs
    for s in range(seqs):
        pick = (
            lax.broadcasted_iota(jnp.int32, (hd, rows), 1)
            == lax.broadcasted_iota(jnp.int32, (hd, rows), 0) * seqs + s
        ).astype(f32).astype(bf16)
        for h in range(heads):
            kv_ref[0, h, s] = jnp.dot(pick, k_ref[h], preferred_element_type=f32).astype(bf16)
            kv_ref[1, h, s] = jnp.dot(pick, v_ref[h], preferred_element_type=f32).astype(bf16)
            query = jnp.dot(pick, q_ref[h], preferred_element_type=f32)
            qt_ref[h, s] = query.T.astype(bf16)

    top = ids_ref.shape[0]
    logits = [logits_ref[k : k + 1] for k in range(top)]
    peak = functools.reduce(jnp.maximum, logits)
    powers = [jnp.exp(value - peak) for value in logits]
    share = 1.0 / functools.reduce(jnp.add, powers)
    slot = lax.broadcasted_iota(jnp.int32, (slots, tokens), 0)
    for group in range(n_ep):
        expert = jnp.where(slot < local_experts, group * local_experts + slot, -1)
        table = jnp.zeros((slots, tokens), f32)
        for k in range(top):
            table = table + jnp.where(ids_ref[k : k + 1] == expert, powers[k] * share, 0.0)
        wt_ref[group] = table
    pl.semaphore_wait(barrier, n_ep - 1 + n_tp - 1)

    mine = pl.ds(pl.multiple_of(core * half, half), half)

    piece = pl.ds(pl.multiple_of(core * half + zp * quarter, quarter), quarter)

    def far(d):
        return sum((d // 2**i) % 2 for i in range(n_ep.bit_length())) > 1

    def x_copy(d, is_far):
        sent = piece if is_far else mine
        return pltpu.make_async_remote_copy(
            src_ref=x_ref.at[sent],
            dst_ref=xr.at[d, sent],
            send_sem=x_ss.at[d],
            recv_sem=x_rs.at[d],
            device_id={"ep": ep_peer(d)},
            device_id_type=MESH,
        )

    def wt_copy(d):
        return pltpu.make_async_remote_copy(
            src_ref=wt_ref.at[ep_peer(d)],
            dst_ref=wr.at[d],
            send_sem=wt_ss.at[d],
            recv_sem=wt_rs.at[d],
            device_id={"ep": ep_peer(d)},
            device_id_type=MESH,
        )

    def g_copy(d):
        return pltpu.make_async_remote_copy(
            src_ref=xr.at[d, piece],
            dst_ref=xr.at[d, piece],
            send_sem=g_ss.at[d],
            recv_sem=g_rs.at[d],
            device_id={"tp": zmate},
            device_id_type=MESH,
        )

    def f_copy(d):
        return pltpu.make_async_remote_copy(
            src_ref=xr.at[d, mine],
            dst_ref=xr.at[d, mine],
            send_sem=f_ss.at[d],
            recv_sem=f_rs.at[d],
            device_id={"tp": mate},
            device_id_type=MESH,
        )

    def kv_copy(d):
        return pltpu.make_async_remote_copy(
            src_ref=kv_ref,
            dst_ref=kvr.at[d],
            send_sem=kv_ss.at[d],
            recv_sem=kv_rs.at[d],
            device_id={"ep": (e + d) % n_ep},
            device_id_type=MESH,
        )

    def c_copy(d):
        return pltpu.make_async_remote_copy(
            src_ref=pb.at[d, 1 - core],
            dst_ref=cr.at[d],
            send_sem=c_ss.at[d],
            recv_sem=c_rs.at[d],
            device_id={"tp": mate},
            device_id_type=MESH,
        )

    def r_copy(d, k):
        c = (zi + k) % zs
        return pltpu.make_async_remote_copy(
            src_ref=sb.at[d, c],
            dst_ref=rr.at[d, c],
            send_sem=r_ss.at[d, k - 1],
            recv_sem=r_rs.at[d, k - 1],
            device_id={"ep": ep_peer(d)},
            device_id_type=MESH,
        )

    def z_copy(d):
        dz = (zi + d) % zs
        return pltpu.make_async_remote_copy(
            src_ref=zb.at[dz],
            dst_ref=zr.at[d],
            send_sem=z_ss.at[d],
            recv_sem=z_rs.at[d],
            device_id={"tp": dz * 2 + core},
            device_id_type=MESH,
        )

    def a_copy(d):
        to = (t + d) % n_tp
        return pltpu.make_async_remote_copy(
            src_ref=at_send.at[to],
            dst_ref=at_recv.at[t],
            send_sem=a_ss.at[d],
            recv_sem=a_rs.at[d],
            device_id={"tp": to},
            device_id_type=MESH,
        )

    for d in range(1, n_ep):
        wt_copy(d).start()
    distances = [d for d in range(1, n_ep) if far(d)]
    near = [d for d in range(1, n_ep) if not far(d)]
    for d in distances + near:
        x_copy(d, far(d)).start()
    for d in range(1, n_ep):

        @pl.when(e + d < n_ep)
        def _():
            kv_copy(d).start()

    def normalize(rows_ref):
        values = rows_ref[...].astype(f32)
        mean = jnp.mean(values * values, axis=-1, keepdims=True)
        xn[...] = (values * lax.rsqrt(mean + norm_eps) * gain_ref[...]).astype(bf16)

    def experts(d, route):
        columns = route.T
        hidden = []
        for j in range(local_experts):
            gate_pre = jnp.dot(xn[...], wg[j], preferred_element_type=f32)
            up_pre = jnp.dot(xn[...], wu[j], preferred_element_type=f32)
            hidden.append(activate(gate_pre, up_pre))
        for c in range(n_tp):
            total = None
            for j in range(local_experts):
                term = columns[:, j : j + 1] * jnp.dot(
                    hidden[j], wd[j, :, c * ch : (c + 1) * ch], preferred_element_type=f32
                )
                total = term if total is None else total + term
            pb[d, c % 2, c // 2] = total.astype(bf16)

    def finish(d, send):
        c_copy(d).wait_recv()
        for k in range(1, zs + 1):
            c = (zi + k) % zs
            sb[d, c] = (pb[d, core, c].astype(f32) + cr[d, c].astype(f32)).astype(bf16)
            if send:
                r_copy(d, k).start()

    pairs = heads * seqs
    row_id = lax.broadcasted_iota(jnp.int32, (seg, seg), 0)
    col_id = lax.broadcasted_iota(jnp.int32, (seg, seg), 1)
    later_mask = (row_id > col_id).astype(f32).astype(bf16)
    scale = hd ** (-0.5)

    def block(kv, diagonal):
        outs = []
        for p in range(pairs):
            h, s = p // seqs, p % seqs
            scores = jnp.dot(qt_ref[h, s], kv[0, h, s], preferred_element_type=f32) * scale
            log_term = jnp.log(1.0 + jnp.exp(-jnp.abs(scores)))
            keep = -(jnp.maximum(scores, 0.0) + log_term)
            beta = jnp.minimum(scores, 0.0) - log_term
            if diagonal:
                keep = jnp.where(col_id < row_id, keep, 0.0)
            high = keep.astype(bf16)
            low = (keep - high.astype(f32)).astype(bf16)
            within = jnp.dot(high, later_mask, preferred_element_type=f32) + jnp.dot(
                low, later_mask, preferred_element_type=f32
            )
            weight = jnp.exp(beta + within)
            if diagonal:
                weight = jnp.where(col_id < row_id, weight, 0.0)
            out = lax.dot_general(
                weight.astype(bf16),
                kv[1, h, s],
                (((1,), (1,)), ((), ())),
                preferred_element_type=f32,
            )
            outs.append((out, jnp.sum(keep, axis=1, keepdims=True)))
        return outs

    for p, (out, total) in enumerate(block(kv_ref, True)):
        acc[p] = out
        tot[p] = total

    normalize(x_ref)
    for d in distances:
        x_copy(d, True).wait_recv()
        g_copy(d).start()
    for copy in weights[:3]:
        copy.wait()
    experts(0, wt_ref[e])
    c_copy(0).start()

    def step(d, carry):
        @pl.when(far(d))
        def _():
            g_copy(d).wait_recv()

        @pl.when(jnp.logical_not(far(d)))
        def _():
            x_copy(d, False).wait_recv()

        f_copy(d).start()

        @pl.when(d == 1)
        def _():
            finish(0, False)

        @pl.when(d > 1)
        def _():
            finish(d - 1, True)

        f_copy(d).wait_recv()
        wt_copy(d).wait_recv()
        normalize(xr.at[d])
        experts(d, wr[d])
        c_copy(d).start()
        return carry

    lax.fori_loop(1, n_ep, step, 0)
    finish(n_ep - 1, True)

    def further(d, carry):
        kv_copy(d).wait_recv()
        for p, (out, total) in enumerate(block(kvr.at[d], False)):
            later = tot[p]
            acc[p] = acc[p] + jnp.exp(later) * out
            tot[p] = later + total
        return carry

    lax.fori_loop(1, e + 1, further, 0)
    for p in range(pairs):
        h, s = p // seqs, p % seqs
        attended = acc[p]
        for c in range(n_tp):
            at_send[c, s * pp : (s + 1) * pp, h * hd : (h + 1) * hd] = attended[
                c * pp : (c + 1) * pp
            ].astype(bf16)
    for d in range(1, n_tp):
        a_copy(d).start()

    own = None
    for k in range(1, zs + 1):
        c = (zi + k) % zs
        own = sb[0, c].astype(f32)
        for d in range(1, n_ep):
            r_copy(d, k).wait_recv()
            own = own + rr[d, c].astype(f32)
        if k < zs:
            zb[c] = own.astype(bf16)
            z_copy(k).start()

    weights[3].wait()
    at_recv[t] = at_send[t]
    for d in range(1, n_tp):
        pltpu.make_async_remote_copy(
            src_ref=at_send.at[t],
            dst_ref=at_recv.at[(t + n_tp - d) % n_tp],
            send_sem=a_ss.at[d],
            recv_sem=a_rs.at[d],
            device_id={"tp": (t + d) % n_tp},
            device_id_type=MESH,
        ).wait_recv()
    channels = heads * hd
    wide = jnp.concatenate([at_recv[c] for c in range(n_tp)], axis=1)
    mixed = jnp.dot(wide, wm[...], preferred_element_type=f32)
    for s in range(seqs):
        mix_out[s] = mixed[s * pp : (s + 1) * pp].astype(bf16)

    total = own
    for d in range(1, zs):
        z_copy(d).wait_recv()
        total = total + zr[d].astype(f32)
    routed_out[...] = total.T.astype(bf16)

    for d in range(1, n_ep):
        x_copy(d, far(d)).wait_send()
        if far(d):
            g_copy(d).wait_send()
        wt_copy(d).wait_send()
        f_copy(d).wait_send()
        for k in range(1, zs + 1):
            r_copy(d, k).wait_send()

        @pl.when(e + d < n_ep)
        def _():
            kv_copy(d).wait_send()

    for d in range(n_ep):
        c_copy(d).wait_send()
    for d in range(1, zs):
        z_copy(d).wait_send()
    for d in range(1, n_tp):
        a_copy(d).wait_send()


def body(
    queries,
    key_vectors,
    value_vectors,
    mixer_weight,
    expert_rows,
    norm_gain,
    route_ids,
    route_logits,
    gate_weight,
    up_weight,
    down_weight,
):
    n_ep, n_tp = lax.axis_size("ep"), lax.axis_size("tp")
    heads, hd, seqs, seg = queries.shape
    tokens, width = expert_rows.shape
    local_experts, _, ff = gate_weight.shape
    zs, ch, pp = n_tp // 2, width // n_tp, seg // n_tp

    top = route_ids.shape[1]
    slots = 8 * -(-local_experts // 8)
    pairs = heads * seqs
    kv_shape = (2, heads, seqs, hd, seg)

    def merged(rows):
        return rows.reshape(heads, hd * seqs, seg)

    vmem = pl.BlockSpec(memory_space=pltpu.VMEM)
    anywhere = pl.BlockSpec(memory_space=pltpu.HBM)
    dma = pltpu.SemaphoreType.DMA
    outs = 2 * seqs * pp * width + 2 * ch * tokens
    limit = (60 * 1024 * 1024) - outs - (64 << 10)
    return pl.pallas_call(
        functools.partial(kernel, n_ep, n_tp),
        out_shape=(
            jax.ShapeDtypeStruct((seqs, pp, width), bf16),
            jax.ShapeDtypeStruct((ch, tokens), bf16),
        ),
        in_specs=[vmem] * 7 + [anywhere] * 4,
        out_specs=(vmem, vmem),
        scratch_shapes=[
            pltpu.VMEM(gate_weight.shape, bf16),
            pltpu.VMEM(up_weight.shape, bf16),
            pltpu.VMEM(down_weight.shape, bf16),
            pltpu.VMEM(mixer_weight.shape, bf16),
            pltpu.VMEM((n_ep, tokens, width), bf16),
            pltpu.VMEM((n_ep, slots, tokens), f32),
            pltpu.VMEM((tokens, width), bf16),
            pltpu.VMEM((n_ep,) + kv_shape, bf16),
            pltpu.VMEM((n_ep, 2, zs, tokens, ch), bf16),
            pltpu.VMEM((n_ep, zs, tokens, ch), bf16),
            pltpu.VMEM((n_ep, zs, tokens, ch), bf16),
            pltpu.VMEM((n_ep, zs, tokens, ch), bf16),
            pltpu.VMEM((zs, tokens, ch), bf16),
            pltpu.VMEM((zs, tokens, ch), bf16),
            pltpu.VMEM((n_tp, seqs * pp, heads * hd), bf16),
            pltpu.VMEM((n_tp, seqs * pp, heads * hd), bf16),
            pltpu.VMEM((heads, seqs, seg, hd), bf16),
            pltpu.VMEM(kv_shape, bf16),
            pltpu.VMEM((n_ep, slots, tokens), f32),
            pltpu.VMEM((pairs, seg, hd), f32),
            pltpu.VMEM((pairs, seg, 1), f32),
            dma((4,)),
        ]
        + [dma((n_ep,))] * 12
        + [dma((n_ep, zs))] * 2
        + [dma((zs,))] * 2
        + [dma((n_tp,))] * 2,
        compiler_params=pltpu.CompilerParams(
            collective_id=0, has_side_effects=True, vmem_limit_bytes=limit
        ),
    )(
        merged(queries),
        merged(key_vectors),
        merged(value_vectors),
        expert_rows,
        norm_gain[None, :],
        route_ids.T,
        route_logits.T,
        gate_weight,
        up_weight,
        down_weight,
        mixer_weight,
    )


def solution(mesh):
    in_specs = (
        P("tp", None, None, "ep"),
        P("tp", None, None, "ep"),
        P("tp", None, None, "ep"),
        P(),
        P("ep", None),
        P(),
        P("ep", None),
        P("ep", None),
        P("ep", None, "tp"),
        P("ep", None, "tp"),
        P("ep", "tp", None),
    )
    out_specs = (P(None, ("ep", "tp"), None), P("tp", "ep"))
    return jax.shard_map(body, mesh=mesh, in_specs=in_specs, out_specs=out_specs, check_vma=False)
```
